32 devices in a mesh: grp: 2 (over y), fs: 4 (over z), tp: 4 (over x, core).
Axes of the slice: x: 2, y: 2, z: 4, core: 2. Of those that a mesh axis runs over, the one named last changes fastest.
Arguments:
- tokens: bfloat16 [8192, 2048], P(('grp', 'fs')), parts along dimension 0, may hold values from -1300 to 1300
- norm_gain: bfloat16 [2048], replicated, may hold values from 0.099609375 to 1.8984375
- gate_weight: bfloat16 [2048, 5120], P('fs', 'tp'), may hold values from -0.125 to 0.125
- up_weight: bfloat16 [2048, 5120], P('fs', 'tp'), may hold values from -0.125 to 0.125
- down_weight: bfloat16 [5120, 2048], P('tp', 'fs'), may hold values from -0.078125 to 0.078125
Outputs:
- mixed: bfloat16 [8192, 2048], P(('grp', 'fs', 'tp')), parts along dimension 0
The draws below stay inside these ranges and needn't reach their ends.
There are 2 independent parts, one for each index of `grp`. The reference program is written for one: setup_inputs(seed, part) draws one part's arguments, and reference() takes and returns one part's arrays. A program takes and returns all parts, laid end to end along the dimension named above; an argument that names none is the same for every part. Nothing has to cross between parts.
All inputs are finite; a program needn't handle non-finite values.
Results may differ from the reference program's by a relative error of at most 0.013.
Values may be sent and summed in bfloat16 or wider, within the bound.
A program may use at most 64 MiB of HBM per device.

```python
import math
import jax
import jax.numpy as jnp
from jax import lax

D = 2048
FF = 5120
TOKENS = 4096
N_TP = 4


def draw_tokens(key, part):
    key_base = jax.random.fold_in(key, 11)
    key_rows = jax.random.fold_in(key, 12)
    key_cols = jax.random.fold_in(key, 13)
    col_scale = jnp.exp(jax.random.uniform(key_cols, (1, D), jnp.float32, 0.0, math.log(10.0)))
    base = jnp.clip(jax.random.normal(key_base, (TOKENS, D), jnp.float32), -5.0, 5.0)
    row_scale = jnp.exp(jax.random.uniform(key_rows, (TOKENS, 1), jnp.float32, 0.0, math.log(10.0)))
    return (base * row_scale * col_scale).astype(jnp.bfloat16)


def level_of(own_key, extent, cuts, least, high):
    def one(dim, shards_of):
        heights = jax.random.uniform(jax.random.fold_in(jax.random.fold_in(own_key, 6), dim), (shards_of,), jnp.float32, least / len(cuts), high / len(cuts))
        return jnp.repeat(jnp.exp(heights), extent[dim] // shards_of).reshape((-1,) + (1,) * (len(extent) - dim - 1))

    factor_of = one(*cuts[0])
    for cut in cuts[1:]:
        factor_of = factor_of * one(*cut)
    return factor_of


def noise(rng, shape, deviation, reach, pieces=(), dtype=jnp.bfloat16):
    result = deviation * jax.random.normal(rng, shape, jnp.float32)
    if pieces:
        result = result * level_of(rng, shape, pieces, -0.22, 0.18)
    return jnp.clip(result, -reach, reach).astype(dtype)


def setup_inputs(seed: int = 0, part: int = 0) -> dict:
    key_list = jax.random.split(jax.random.key(seed), 6)
    part_keys = jax.random.split(jax.random.fold_in(key_list[5], part), 6)
    return {
        "tokens": draw_tokens(jax.random.fold_in(jax.random.fold_in(key_list[5], part), 71), part),
        "norm_gain": jnp.clip(1.0 + 0.18 * jax.random.normal(key_list[1], (D,), jnp.float32), 0.099609375, 1.8984375).astype(jnp.bfloat16),
        "gate_weight": noise(key_list[2], (D, FF), D ** -0.5, 0.125, ((0, 4), (1, 4))),
        "up_weight": noise(key_list[3], (D, FF), D ** -0.5, 0.125, ((0, 4), (1, 4))),
        "down_weight": noise(key_list[4], (FF, D), FF ** -0.5, 0.078125, ((0, 4), (1, 4))),
    }


EPSILON = 1e-06

def reference(tokens, norm_gain, gate_weight, up_weight, down_weight):
    as_float = tokens.astype(jnp.float32)
    scale = lax.rsqrt(lax.optimization_barrier(jnp.mean(as_float * as_float, axis=-1, keepdims=True)) + EPSILON)
    normed = (as_float * scale * norm_gain.astype(jnp.float32)).astype(jnp.bfloat16)
    gate_acts = jnp.dot(normed, gate_weight, preferred_element_type=jnp.float32)
    up_acts = jnp.dot(normed, up_weight, preferred_element_type=jnp.float32)
    hidden = (jax.nn.silu(gate_acts) * up_acts).astype(jnp.bfloat16)
    group_width = FF // N_TP
    hidden_groups = jnp.transpose(hidden.reshape(TOKENS, N_TP, group_width), (1, 0, 2))
    down_groups = down_weight.reshape(N_TP, group_width, D)

    def accumulate(running, pair):
        hidden_part, weight_part = pair
        product = jnp.dot(hidden_part, weight_part, preferred_element_type=jnp.float32)
        partials = lax.optimization_barrier(product.astype(jnp.bfloat16)).astype(jnp.float32)
        return (running + partials, None)
    running, _ = lax.scan(accumulate, jnp.zeros((TOKENS, D), jnp.float32), (hidden_groups, down_groups))
    return running.astype(jnp.bfloat16)
```

```python
import functools

import jax
import jax.numpy as jnp
from jax import lax
from jax.experimental import pallas as pl
from jax.experimental.pallas import tpu as pltpu
from jax.sharding import PartitionSpec as P

EPSILON = 1e-06
MESH = pl.DeviceIdType.MESH
CORES = 2
VMEM_BYTES = 64 * 1024 * 1024 - 128 * 1024


def wrapped(value, size):
    return lax.rem(value, size)


def kernel(
    groups, n, chips, cuts,
    tok, gain, gu, dn, out,
    gbuf, dbuf, theirs, normed, hidden, keep, psend, precv, asend, arecv,
    gu_sent, gu_came, dn_sent, dn_came, tok_sent, tok_came, relay_sent, relay_came,
    pair_sent, pair_came, mix_sent, mix_came, local_sem,
):
    y, z, tp = lax.axis_index("grp"), lax.axis_index("fs"), lax.axis_index("tp")
    core, x = lax.rem(tp, CORES), lax.div(tp, CORES)
    partner = tp + 1 - 2 * core
    above, below = wrapped(z + 1, n), wrapped(z + n - 1, n)
    has_above, has_below = z < n - 1, z > 0

    rows, width = tok.shape
    depth, half = gu.shape[0], rows // 2
    units = dn.shape[0]
    columns = dn.shape[1]
    piece = depth // cuts
    own_rows = rows // (chips * CORES)
    peers = [(i, dx) for i in range(groups) for dx in range(chips) if (i, dx) != (0, 0)]

    def peer(i, dx):
        return wrapped(y + i, groups), wrapped(x + dx, chips)

    barrier = pltpu.get_barrier_semaphore()

    def greet(device):
        pl.semaphore_signal(barrier, inc=1, device_id=device, device_id_type=MESH)

    @pl.when(has_below)
    def _():
        greet({"fs": below})

    @pl.when(has_above)
    def _():
        greet({"fs": above})

    greet({"tp": partner})
    for i, dx in peers:
        g, xx = peer(i, dx)
        greet({"grp": g, "tp": CORES * xx + core})
    along_z = lax.div(z + n - 1, n) + lax.div(2 * n - 2 - z, n)
    pl.semaphore_wait(barrier, 1 + len(peers) + along_z)

    def gu_copy(slot, cut, direction, own=False):
        there = gbuf.at[pl.ds(pl.multiple_of(slot * depth + cut * piece, piece), piece)]
        index = slot * cuts + cut
        return pltpu.make_async_remote_copy(
            src_ref=gu.at[pl.ds(cut * piece, piece)] if own else there,
            dst_ref=there,
            send_sem=gu_sent.at[direction * n * cuts + index],
            recv_sem=gu_came.at[index],
            device_id={"fs": below if direction else above},
            device_id_type=MESH,
        )

    def dn_copy(slot, direction, own=False):
        return pltpu.make_async_remote_copy(
            src_ref=dn if own else dbuf.at[slot],
            dst_ref=dbuf.at[slot],
            send_sem=dn_sent.at[direction * n + slot],
            recv_sem=dn_came.at[slot],
            device_id={"fs": below if direction else above},
            device_id_type=MESH,
        )

    def tok_copy(i):
        part = pl.ds(pl.multiple_of(core * half, half), half)
        return pltpu.make_async_remote_copy(
            src_ref=tok.at[part],
            dst_ref=theirs.at[i - 1, part],
            send_sem=tok_sent.at[i - 1],
            recv_sem=tok_came.at[i - 1],
            device_id={"grp": wrapped(y + i, groups)},
            device_id_type=MESH,
        )

    def relay_copy(i):
        part = theirs.at[i - 1, pl.ds(pl.multiple_of(core * half, half), half)]
        return pltpu.make_async_remote_copy(
            src_ref=part,
            dst_ref=part,
            send_sem=relay_sent.at[i - 1],
            recv_sem=relay_came.at[i - 1],
            device_id={"tp": partner},
            device_id_type=MESH,
        )

    for cut in range(cuts):

        @pl.when(has_above)
        def _(cut=cut):
            gu_copy(z, cut, 0, own=True).start()

        @pl.when(has_below)
        def _(cut=cut):
            gu_copy(z, cut, 1, own=True).start()

    @pl.when(z == 0)
    def _():
        dn_copy(z, 0, own=True).start()

    @pl.when(z == n - 1)
    def _():
        dn_copy(z, 1, own=True).start()

    for i in range(1, groups):
        tok_copy(i).start()
    own_gu = pltpu.make_async_copy(
        gu, gbuf.at[pl.ds(pl.multiple_of(z * depth, depth), depth)], local_sem.at[0]
    )
    own_dn = pltpu.make_async_copy(dn, dbuf.at[z], local_sem.at[1])
    own_gu.start()
    own_dn.start()

    gains = gain[...].astype(jnp.float32)
    tile = 32

    def normalize(source, first):
        def step(t, carry):
            values = source[pl.ds(pl.multiple_of(t * tile, tile), tile), :].astype(jnp.float32)
            scale = lax.rsqrt(jnp.mean(values * values, axis=-1, keepdims=True) + EPSILON)
            normed[pl.ds(pl.multiple_of(first + t * tile, tile), tile), :] = (
                values * scale * gains
            ).astype(jnp.bfloat16)
            return carry

        lax.fori_loop(0, rows // tile, step, 0)

    normalize(tok, y * rows)

    def gather(s, carry):
        for cut in range(cuts):

            @pl.when(z >= s)
            def _(cut=cut):
                copy = gu_copy(z - s, cut, 0)
                copy.wait_recv()

                @pl.when(has_above)
                def _():
                    copy.start()

            @pl.when(z + s < n)
            def _(cut=cut):
                copy = gu_copy(z + s, cut, 1)
                copy.wait_recv()

                @pl.when(has_below)
                def _():
                    copy.start()

        @pl.when((s == z) & has_above)
        def _():
            dn_copy(z, 0, own=True).start()

        @pl.when((s == n - 1 - z) & has_below)
        def _():
            dn_copy(z, 1, own=True).start()

        return carry

    gather(1, 0)
    for i in range(1, groups):
        tok_copy(i).wait_recv()
        relay_copy(i).start()
    for i in range(1, groups):
        relay_copy(i).wait_recv()
        normalize(theirs.at[i - 1], wrapped(y + groups - i, groups) * rows)
    lax.fori_loop(2, n, gather, 0)
    own_gu.wait()
    own_dn.wait()

    tall = 512 if (groups * rows) % 512 == 0 else own_rows

    def activate(t, carry):
        where = pl.ds(pl.multiple_of(t * tall, tall), tall)
        mine = normed[where, :]
        gate_acts = jnp.dot(mine, gbuf[:, :units], preferred_element_type=jnp.float32)
        up_acts = jnp.dot(mine, gbuf[:, units:], preferred_element_type=jnp.float32)
        hidden[where, :] = (gate_acts / (1.0 + jnp.exp(-gate_acts)) * up_acts).astype(jnp.bfloat16)
        return carry

    lax.fori_loop(0, groups * rows // tall, activate, 0)

    def pair_copy(slot):
        return pltpu.make_async_remote_copy(
            src_ref=psend.at[slot],
            dst_ref=precv.at[slot],
            send_sem=pair_sent.at[slot],
            recv_sem=pair_came.at[slot],
            device_id={"tp": partner},
            device_id_type=MESH,
        )

    def mix_copy(slot, r):
        g, xx = peer(*peers[r])
        return pltpu.make_async_remote_copy(
            src_ref=asend.at[slot, g * chips + xx],
            dst_ref=arecv.at[slot, r],
            send_sem=mix_sent.at[slot * len(peers) + r],
            recv_sem=mix_came.at[slot * len(peers) + r],
            device_id={"grp": g, "tp": CORES * xx + core},
            device_id_type=MESH,
        )

    def product(slot, j, which):
        first = (CORES * j + which) * own_rows
        block = hidden[pl.ds(pl.multiple_of(first, own_rows), own_rows), :]
        return jnp.dot(block, dbuf[slot], preferred_element_type=jnp.float32)

    def block_of(slot):
        def give(j, carry):
            psend[slot, j] = product(slot, j, 1 - core).astype(jnp.bfloat16)
            return carry

        lax.fori_loop(0, groups * chips, give, 0)
        pair_copy(slot).start()

        def hold(j, carry):
            keep[j] = product(slot, j, core)
            return carry

        lax.fori_loop(0, groups * chips, hold, 0)
        pair_copy(slot).wait_recv()

        def add(j, carry):
            asend[slot, j] = (keep[j] + precv[slot, j].astype(jnp.float32)).astype(jnp.bfloat16)
            return carry

        lax.fori_loop(0, groups * chips, add, 0)
        for r in range(len(peers)):
            mix_copy(slot, r).start()

    def project(s, carry):
        @pl.when(z >= s)
        def _():
            copy = dn_copy(z - s, 0)
            copy.wait_recv()

            @pl.when(has_above)
            def _():
                copy.start()

            block_of(z - s)

        @pl.when(z + s < n)
        def _():
            copy = dn_copy(z + s, 1)
            copy.wait_recv()

            @pl.when(has_below)
            def _():
                copy.start()

            block_of(z + s)

        return carry

    block_of(z)
    lax.fori_loop(1, n, project, 0)

    def finish(slot):
        for r in range(len(peers)):
            mix_copy(slot, r).wait_recv()
        total = asend[slot, y * chips + x].astype(jnp.float32)
        for r in range(len(peers)):
            total = total + arecv[slot, r].astype(jnp.float32)
        out[:, pl.ds(pl.multiple_of(slot * columns, columns), columns)] = total.astype(jnp.bfloat16)

    def finish_step(s, carry):
        @pl.when(z >= s)
        def _():
            finish(z - s)

        @pl.when(z + s < n)
        def _():
            finish(z + s)

        return carry

    finish(z)
    lax.fori_loop(1, n, finish_step, 0)

    def left(slot, carry):
        @pl.when((slot <= z) & has_above)
        def _():
            for cut in range(cuts):
                gu_copy(slot, cut, 0).wait_send()
            dn_copy(slot, 0).wait_send()

        @pl.when((slot >= z) & has_below)
        def _():
            for cut in range(cuts):
                gu_copy(slot, cut, 1).wait_send()
            dn_copy(slot, 1).wait_send()

        pair_copy(slot).wait_send()
        for r in range(len(peers)):
            mix_copy(slot, r).wait_send()
        return carry

    lax.fori_loop(0, n, left, 0)
    for i in range(1, groups):
        tok_copy(i).wait_send()
        relay_copy(i).wait_send()


def on_device(groups, n, devices, tokens, norm_gain, gate_weight, up_weight, down_weight):
    chips, cuts = devices // CORES, 2
    rows, width = tokens.shape
    depth, columns = gate_weight.shape[0], down_weight.shape[1]
    share = gate_weight.shape[1] // groups
    units = -(-share // 128) * 128
    first = lax.axis_index("grp") * share

    def mine(weight, dim):
        part = lax.dynamic_slice_in_dim(weight, first, share, dim)
        short = [(0, units - share) if d == dim else (0, 0) for d in range(2)]
        return jnp.pad(part, short) if units > share else part

    gu = jnp.concatenate([mine(gate_weight, 1), mine(up_weight, 1)], axis=1)
    dn = mine(down_weight, 0)
    own_rows = rows // devices
    places, peers = groups * chips, groups * chips - 1
    bf16, f32, dma = jnp.bfloat16, jnp.float32, pltpu.SemaphoreType.DMA
    return pl.pallas_call(
        functools.partial(kernel, groups, n, chips, cuts),
        out_shape=jax.ShapeDtypeStruct((own_rows, width), bf16),
        in_specs=[pl.BlockSpec(memory_space=pltpu.VMEM)] * 4,
        out_specs=pl.BlockSpec(memory_space=pltpu.VMEM),
        scratch_shapes=[
            pltpu.VMEM((n * depth, 2 * units), bf16),
            pltpu.VMEM((n, units, columns), bf16),
            pltpu.VMEM((groups - 1, rows, width), bf16),
            pltpu.VMEM((groups * rows, width), bf16),
            pltpu.VMEM((groups * rows, units), bf16),
            pltpu.VMEM((places, own_rows, columns), f32),
            pltpu.VMEM((n, places, own_rows, columns), bf16),
            pltpu.VMEM((n, places, own_rows, columns), bf16),
            pltpu.VMEM((n, places, own_rows, columns), bf16),
            pltpu.VMEM((n, peers, own_rows, columns), bf16),
            dma((2 * n * cuts,)),
            dma((n * cuts,)),
            dma((2 * n,)),
            dma((n,)),
            dma((groups - 1,)),
            dma((groups - 1,)),
            dma((groups - 1,)),
            dma((groups - 1,)),
            dma((n,)),
            dma((n,)),
            dma((n * peers,)),
            dma((n * peers,)),
            dma((2,)),
        ],
        compiler_params=pltpu.CompilerParams(
            collective_id=0, has_side_effects=True, vmem_limit_bytes=VMEM_BYTES - 2**20
        ),
    )(tokens, norm_gain.reshape(1, width), gu, dn)


def solution(mesh):
    sizes = mesh.shape
    return jax.shard_map(
        functools.partial(on_device, sizes["grp"], sizes["fs"], sizes["tp"]),
        mesh=mesh,
        in_specs=(P(("grp", "fs"), None), P(), P("fs", "tp"), P("fs", "tp"), P("tp", "fs")),
        out_specs=P(("grp", "fs", "tp"), None),
        check_vma=False,
    )
```

```python
import functools

import jax
import jax.numpy as jnp
from jax import lax
from jax.experimental import pallas as pl
from jax.experimental.pallas import tpu as pltpu
from jax.sharding import PartitionSpec as P

EPSILON = 1e-06
MESH = pl.DeviceIdType.MESH
CORES = 2
VMEM_BYTES = 64 * 1024 * 1024 - 128 * 1024


def wrapped(value, size):
    return lax.rem(value, size)


def kernel(
    groups, n, chips, parts, sliced,
    tok, gain, gate, up, dn, out,
    gbuf, dbuf, raw, normed, acc, hidden, keep, psend, precv, asend, arecv,
    gu_sent, gu_came, dn_sent, dn_came, tok_sent, tok_came, relay_sent, relay_came,
    pair_sent, pair_came, mix_sent, mix_came, local_sem,
):
    y, z, tp = lax.axis_index("grp"), lax.axis_index("fs"), lax.axis_index("tp")
    core, x = lax.rem(tp, CORES), lax.div(tp, CORES)
    partner = tp + 1 - 2 * core
    above, below = wrapped(z + 1, n), wrapped(z + n - 1, n)
    has_above, has_below = z < n - 1, z > 0

    rows, width = tok.shape
    depth, half = gate.shape[0], rows // 2
    units = gbuf.shape[2]
    columns = dbuf.shape[2]
    own_rows = rows // (chips * CORES)
    first = 0 if sliced else pl.multiple_of(y * units, units)
    mine = (gate.at[:, pl.ds(first, units)], up.at[:, pl.ds(first, units)])
    places = groups * chips
    peers = [(i, dx) for i in range(groups) for dx in range(chips) if (i, dx) != (0, 0)]

    def peer(i, dx):
        return wrapped(y + i, groups), wrapped(x + dx, chips)

    def rows_of(slot):
        return pl.ds(pl.multiple_of(slot * depth, depth), depth)

    def own_dn(h):
        return dn.at[pl.ds(first, units), pl.ds(h * columns, columns)]

    locals_ = [pltpu.make_async_copy(tok, raw.at[0], local_sem.at[0])]
    for k in range(2):
        locals_.append(
            pltpu.make_async_copy(mine[k], gbuf.at[k, rows_of(z)], local_sem.at[1 + k])
        )
    for h in range(parts):
        locals_.append(
            pltpu.make_async_copy(own_dn(h), dbuf.at[z * parts + h], local_sem.at[3 + h])
        )
    for copy in locals_:
        copy.start()

    barrier = pltpu.get_barrier_semaphore()

    def greet(device):
        pl.semaphore_signal(barrier, inc=1, device_id=device, device_id_type=MESH)

    @pl.when(has_below)
    def _():
        greet({"fs": below})

    @pl.when(has_above)
    def _():
        greet({"fs": above})

    greet({"tp": partner})
    for i, dx in peers:
        g, xx = peer(i, dx)
        greet({"grp": g, "tp": CORES * xx + core})
    along_z = lax.div(z + n - 1, n) + lax.div(2 * n - 2 - z, n)
    pl.semaphore_wait(barrier, 1 + len(peers) + along_z)

    def gu_copy(slot, k, direction, own=False):
        there = gbuf.at[k, rows_of(slot)]
        index = slot * 2 + k
        return pltpu.make_async_remote_copy(
            src_ref=mine[k] if own else there,
            dst_ref=there,
            send_sem=gu_sent.at[direction * n * 2 + index],
            recv_sem=gu_came.at[index],
            device_id={"fs": below if direction else above},
            device_id_type=MESH,
        )

    def dn_copy(slot, h, direction, own=False):
        index = slot * parts + h
        return pltpu.make_async_remote_copy(
            src_ref=own_dn(h) if own else dbuf.at[index],
            dst_ref=dbuf.at[index],
            send_sem=dn_sent.at[direction * n * parts + index],
            recv_sem=dn_came.at[index],
            device_id={"fs": below if direction else above},
            device_id_type=MESH,
        )

    def start_own_dn(direction):
        for h in range(parts):
            dn_copy(z, h, direction, own=True).start()

    def tok_copy(i):
        part = pl.ds(pl.multiple_of(core * half, half), half)
        return pltpu.make_async_remote_copy(
            src_ref=tok.at[part],
            dst_ref=raw.at[i, part],
            send_sem=tok_sent.at[i - 1],
            recv_sem=tok_came.at[i - 1],
            device_id={"grp": wrapped(y + i, groups)},
            device_id_type=MESH,
        )

    def relay_copy(i):
        part = raw.at[i, pl.ds(pl.multiple_of(core * half, half), half)]
        return pltpu.make_async_remote_copy(
            src_ref=part,
            dst_ref=part,
            send_sem=relay_sent.at[i - 1],
            recv_sem=relay_came.at[i - 1],
            device_id={"tp": partner},
            device_id_type=MESH,
        )

    for k in range(2):

        @pl.when(has_above)
        def _(k=k):
            gu_copy(z, k, 0, own=True).start()

        @pl.when(has_below)
        def _(k=k):
            gu_copy(z, k, 1, own=True).start()

    for i in range(1, groups):
        tok_copy(i).start()

    @pl.when(z == 0)
    def _():
        start_own_dn(0)

    @pl.when(z == n - 1)
    def _():
        start_own_dn(1)

    gains = gain[...].astype(jnp.float32)
    tile = 32

    def normalize(i, first_row):
        def step(t, carry):
            where = pl.ds(pl.multiple_of(t * tile, tile), tile)
            values = raw[i, where, :].astype(jnp.float32)
            scale = lax.rsqrt(jnp.mean(values * values, axis=-1, keepdims=True) + EPSILON)
            normed[pl.ds(pl.multiple_of(first_row + t * tile, tile), tile), :] = (
                values * scale * gains
            ).astype(jnp.bfloat16)
            return carry

        lax.fori_loop(0, rows // tile, step, 0)

    for copy in locals_:
        copy.wait()
    normalize(0, y * rows)

    def gather(s):
        for k in range(2):

            @pl.when(z >= s)
            def _(k=k):
                copy = gu_copy(z - s, k, 0)
                copy.wait_recv()

                @pl.when(has_above)
                def _():
                    copy.start()

            @pl.when(z + s < n)
            def _(k=k):
                copy = gu_copy(z + s, k, 1)
                copy.wait_recv()

                @pl.when(has_below)
                def _():
                    copy.start()

        @pl.when((s == z) & has_above)
        def _():
            start_own_dn(0)

        @pl.when((s == n - 1 - z) & has_below)
        def _():
            start_own_dn(1)

    total_rows = groups * rows
    tall = 512 if total_rows % 512 == 0 else own_rows

    def term(slot, opening):
        some = pl.ds(pl.multiple_of(slot * depth, depth), depth)

        def step(t, carry):
            where = pl.ds(pl.multiple_of(t * tall, tall), tall)
            for k in range(2):
                value = jnp.dot(normed[where, some], gbuf[k, some, :], preferred_element_type=jnp.float32)
                if opening:
                    acc[k, where, :] = value
                else:
                    acc[k, where, :] += value
            return carry

        lax.fori_loop(0, total_rows // tall, step, 0)

    def terms(s):
        @pl.when(z >= s)
        def _():
            term(z - s, False)

        @pl.when(z + s < n)
        def _():
            term(z + s, False)

    gather(1)
    for i in range(1, groups):
        tok_copy(i).wait_recv()
        relay_copy(i).start()
    for i in range(1, groups):
        relay_copy(i).wait_recv()
        normalize(i, wrapped(y + groups - i, groups) * rows)
    term(z, True)
    if n > 2:
        gather(2)
    terms(1)
    if n > 2:
        terms(2)

    def later(s, carry):
        gather(s)
        terms(s)
        return carry

    lax.fori_loop(3, n, later, 0)

    def activate(t, carry):
        where = pl.ds(pl.multiple_of(t * tile, tile), tile)
        gate_acts = acc[0, where, :]
        hidden[where, :] = (gate_acts / (1.0 + jnp.exp(-gate_acts)) * acc[1, where, :]).astype(
            jnp.bfloat16
        )
        return carry

    lax.fori_loop(0, total_rows // tile, activate, 0)

    def pair_copy(slot):
        return pltpu.make_async_remote_copy(
            src_ref=psend.at[slot],
            dst_ref=precv.at[slot],
            send_sem=pair_sent.at[slot],
            recv_sem=pair_came.at[slot],
            device_id={"tp": partner},
            device_id_type=MESH,
        )

    def mix_copy(slot, r):
        g, xx = peer(*peers[r])
        return pltpu.make_async_remote_copy(
            src_ref=asend.at[slot, g * chips + xx],
            dst_ref=arecv.at[slot, r],
            send_sem=mix_sent.at[slot * len(peers) + r],
            recv_sem=mix_came.at[slot * len(peers) + r],
            device_id={"grp": g, "tp": CORES * xx + core},
            device_id_type=MESH,
        )

    def product(slot, j, which):
        first = (CORES * j + which) * own_rows
        block = hidden[pl.ds(pl.multiple_of(first, own_rows), own_rows), :]
        return jnp.dot(block, dbuf[slot], preferred_element_type=jnp.float32)

    def block_of(slot):
        def give(j, carry):
            psend[slot, j] = product(slot, j, 1 - core).astype(jnp.bfloat16)
            return carry

        lax.fori_loop(0, groups * chips, give, 0)
        pair_copy(slot).start()

        def hold(j, carry):
            keep[j] = product(slot, j, core)
            return carry

        lax.fori_loop(0, groups * chips, hold, 0)
        pair_copy(slot).wait_recv()

        def add(j, carry):
            asend[slot, j] = (keep[j] + precv[slot, j].astype(jnp.float32)).astype(jnp.bfloat16)
            return carry

        lax.fori_loop(0, groups * chips, add, 0)
        for r in range(len(peers)):
            mix_copy(slot, r).start()

    def project(s, carry):
        @pl.when(z >= s)
        def _():
            for h in range(parts):
                copy = dn_copy(z - s, h, 0)
                copy.wait_recv()

                @pl.when(has_above)
                def _():
                    copy.start()

                block_of((z - s) * parts + h)

        @pl.when(z + s < n)
        def _():
            for h in range(parts):
                copy = dn_copy(z + s, h, 1)
                copy.wait_recv()

                @pl.when(has_below)
                def _():
                    copy.start()

                block_of((z + s) * parts + h)

        return carry

    for h in range(parts):
        block_of(z * parts + h)
    lax.fori_loop(1, n, project, 0)

    def finish(slot):
        for r in range(len(peers)):
            mix_copy(slot, r).wait_recv()
        total = asend[slot, y * chips + x].astype(jnp.float32)
        for r in range(len(peers)):
            total = total + arecv[slot, r].astype(jnp.float32)
        out[:, pl.ds(pl.multiple_of(slot * columns, columns), columns)] = total.astype(jnp.bfloat16)

    def finish_step(s, carry):
        @pl.when(z >= s)
        def _():
            for h in range(parts):
                finish((z - s) * parts + h)

        @pl.when(z + s < n)
        def _():
            for h in range(parts):
                finish((z + s) * parts + h)

        return carry

    for h in range(parts):
        finish(z * parts + h)
    lax.fori_loop(1, n, finish_step, 0)

    def left(slot, carry):
        @pl.when((slot <= z) & has_above)
        def _():
            for k in range(2):
                gu_copy(slot, k, 0).wait_send()
            for h in range(parts):
                dn_copy(slot, h, 0).wait_send()

        @pl.when((slot >= z) & has_below)
        def _():
            for k in range(2):
                gu_copy(slot, k, 1).wait_send()
            for h in range(parts):
                dn_copy(slot, h, 1).wait_send()

        for h in range(parts):
            pair_copy(slot * parts + h).wait_send()
            for r in range(len(peers)):
                mix_copy(slot * parts + h, r).wait_send()
        return carry

    lax.fori_loop(0, n, left, 0)
    for i in range(1, groups):
        tok_copy(i).wait_send()
        relay_copy(i).wait_send()


def on_device(groups, n, devices, tokens, norm_gain, gate_weight, up_weight, down_weight):
    chips = devices // CORES
    rows, width = tokens.shape
    depth, columns = gate_weight.shape[0], down_weight.shape[1]
    parts = 2 if columns % 256 == 0 else 1
    columns //= parts
    share = gate_weight.shape[1] // groups
    units = -(-share // 128) * 128
    sliced = units > share
    if sliced:
        first = lax.axis_index("grp") * share

        def mine(weight, dim):
            part = lax.dynamic_slice_in_dim(weight, first, share, dim)
            return jnp.pad(part, [(0, units - share) if d == dim else (0, 0) for d in range(2)])

        gate_weight, up_weight = mine(gate_weight, 1), mine(up_weight, 1)
        down_weight = mine(down_weight, 0)
    own_rows = rows // devices
    places, peers, blocks = groups * chips, groups * chips - 1, n * parts
    bf16, f32, dma = jnp.bfloat16, jnp.float32, pltpu.SemaphoreType.DMA
    far, near = pl.BlockSpec(memory_space=pl.ANY), pl.BlockSpec(memory_space=pltpu.VMEM)
    return pl.pallas_call(
        functools.partial(kernel, groups, n, chips, parts, sliced),
        out_shape=jax.ShapeDtypeStruct((own_rows, width), bf16),
        in_specs=[far, near, far, far, far],
        out_specs=near,
        scratch_shapes=[
            pltpu.VMEM((2, n * depth, units), bf16),
            pltpu.VMEM((blocks, units, columns), bf16),
            pltpu.VMEM((groups, rows, width), bf16),
            pltpu.VMEM((groups * rows, width), bf16),
            pltpu.VMEM((2, groups * rows, units), f32),
            pltpu.VMEM((groups * rows, units), bf16),
            pltpu.VMEM((places, own_rows, columns), f32),
            pltpu.VMEM((blocks, places, own_rows, columns), bf16),
            pltpu.VMEM((blocks, places, own_rows, columns), bf16),
            pltpu.VMEM((blocks, places, own_rows, columns), bf16),
            pltpu.VMEM((blocks, peers, own_rows, columns), bf16),
            dma((2 * n * 2,)),
            dma((n * 2,)),
            dma((2 * blocks,)),
            dma((blocks,)),
            dma((groups - 1,)),
            dma((groups - 1,)),
            dma((groups - 1,)),
            dma((groups - 1,)),
            dma((blocks,)),
            dma((blocks,)),
            dma((blocks * peers,)),
            dma((blocks * peers,)),
            dma((3 + parts,)),
        ],
        compiler_params=pltpu.CompilerParams(
            collective_id=0, has_side_effects=True, vmem_limit_bytes=VMEM_BYTES - 2**20
        ),
    )(tokens, norm_gain.reshape(1, width), gate_weight, up_weight, down_weight)


def solution(mesh):
    sizes = mesh.shape
    return jax.shard_map(
        functools.partial(on_device, sizes["grp"], sizes["fs"], sizes["tp"]),
        mesh=mesh,
        in_specs=(P(("grp", "fs"), None), P(), P("fs", "tp"), P("fs", "tp"), P("tp", "fs")),
        out_specs=P(("grp", "fs", "tp"), None),
        check_vma=False,
    )
```

```python
import functools

import jax
import jax.numpy as jnp
from jax import lax
from jax.experimental import pallas as pl
from jax.experimental.pallas import tpu as pltpu
from jax.sharding import PartitionSpec as P

EPSILON = 1e-06
MESH = pl.DeviceIdType.MESH
CORES = 2
VMEM_BYTES = 64 * 1024 * 1024 - 128 * 1024


def wrapped(value, size):
    return lax.rem(value, size)


def kernel(
    groups, n, chips, parts, sliced,
    tok, gain, gate, up, dn, out,
    gbuf, dbuf, raw, normed, acc, hidden, keep, psend, precv, asend, arecv,
    gu_sent, gu_came, dn_sent, dn_came, tok_sent, tok_came, relay_sent, relay_came,
    pair_sent, pair_came, mix_sent, mix_came, local_sem,
):
    y, z, tp = lax.axis_index("grp"), lax.axis_index("fs"), lax.axis_index("tp")
    core, x = lax.rem(tp, CORES), lax.div(tp, CORES)
    partner = tp + 1 - 2 * core
    above, below = wrapped(z + 1, n), wrapped(z + n - 1, n)
    has_above, has_below = z < n - 1, z > 0

    rows, width = tok.shape
    depth, half = gate.shape[0], rows // 2
    units = gbuf.shape[2]
    columns = dbuf.shape[2]
    own_rows = rows // (chips * CORES)
    first = 0 if sliced else pl.multiple_of(y * units, units)
    mine = (gate.at[:, pl.ds(first, units)], up.at[:, pl.ds(first, units)])
    places = groups * chips
    peers = [(i, dx) for i in range(groups) for dx in range(chips) if (i, dx) != (0, 0)]

    def peer(i, dx):
        return wrapped(y + i, groups), wrapped(x + dx, chips)

    def rows_of(slot):
        return pl.ds(pl.multiple_of(slot * depth, depth), depth)

    def own_dn(h):
        return dn.at[pl.ds(first, units), pl.ds(h * columns, columns)]

    locals_ = [pltpu.make_async_copy(tok, raw.at[0], local_sem.at[0])]
    for k in range(2):
        locals_.append(
            pltpu.make_async_copy(mine[k], gbuf.at[k, rows_of(z)], local_sem.at[1 + k])
        )
    for h in range(parts):
        locals_.append(
            pltpu.make_async_copy(own_dn(h), dbuf.at[z * parts + h], local_sem.at[3 + h])
        )
    for copy in locals_:
        copy.start()

    barrier = pltpu.get_barrier_semaphore()

    def greet(device):
        pl.semaphore_signal(barrier, inc=1, device_id=device, device_id_type=MESH)

    @pl.when(has_below)
    def _():
        greet({"fs": below})

    @pl.when(has_above)
    def _():
        greet({"fs": above})

    greet({"tp": partner})
    for i, dx in peers:
        g, xx = peer(i, dx)
        greet({"grp": g, "tp": CORES * xx + core})
    along_z = lax.div(z + n - 1, n) + lax.div(2 * n - 2 - z, n)
    pl.semaphore_wait(barrier, 1 + len(peers) + along_z)

    def gu_copy(slot, k, direction, own=False):
        there = gbuf.at[k, rows_of(slot)]
        index = slot * 2 + k
        return pltpu.make_async_remote_copy(
            src_ref=mine[k] if own else there,
            dst_ref=there,
            send_sem=gu_sent.at[direction * n * 2 + index],
            recv_sem=gu_came.at[index],
            device_id={"fs": below if direction else above},
            device_id_type=MESH,
        )

    def dn_copy(slot, h, direction, own=False):
        index = slot * parts + h
        return pltpu.make_async_remote_copy(
            src_ref=own_dn(h) if own else dbuf.at[index],
            dst_ref=dbuf.at[index],
            send_sem=dn_sent.at[direction * n * parts + index],
            recv_sem=dn_came.at[index],
            device_id={"fs": below if direction else above},
            device_id_type=MESH,
        )

    def start_own_dn(direction):
        for h in range(parts):
            dn_copy(z, h, direction, own=True).start()

    def tok_copy(i):
        part = pl.ds(pl.multiple_of(core * half, half), half)
        return pltpu.make_async_remote_copy(
            src_ref=tok.at[part],
            dst_ref=raw.at[i, part],
            send_sem=tok_sent.at[i - 1],
            recv_sem=tok_came.at[i - 1],
            device_id={"grp": wrapped(y + i, groups)},
            device_id_type=MESH,
        )

    def relay_copy(i):
        part = raw.at[i, pl.ds(pl.multiple_of(core * half, half), half)]
        return pltpu.make_async_remote_copy(
            src_ref=part,
            dst_ref=part,
            send_sem=relay_sent.at[i - 1],
            recv_sem=relay_came.at[i - 1],
            device_id={"tp": partner},
            device_id_type=MESH,
        )

    for k in range(2):

        @pl.when(has_above)
        def _(k=k):
            gu_copy(z, k, 0, own=True).start()

        @pl.when(has_below)
        def _(k=k):
            gu_copy(z, k, 1, own=True).start()

    for i in range(1, groups):
        tok_copy(i).start()

    @pl.when(z == 0)
    def _():
        start_own_dn(0)

    @pl.when(z == n - 1)
    def _():
        start_own_dn(1)

    gains = gain[...].astype(jnp.float32)
    tile = 32

    def normalize(i, first_row):
        def step(t, carry):
            where = pl.ds(pl.multiple_of(t * tile, tile), tile)
            values = raw[i, where, :].astype(jnp.float32)
            scale = lax.rsqrt(jnp.mean(values * values, axis=-1, keepdims=True) + EPSILON)
            normed[pl.ds(pl.multiple_of(first_row + t * tile, tile), tile), :] = (
                values * scale * gains
            ).astype(jnp.bfloat16)
            return carry

        lax.fori_loop(0, rows // tile, step, 0)

    for copy in locals_:
        copy.wait()
    normalize(0, y * rows)

    def gather(s, kinds=(0, 1)):
        for k in kinds:

            @pl.when(z >= s)
            def _(k=k):
                copy = gu_copy(z - s, k, 0)
                copy.wait_recv()

                @pl.when(has_above)
                def _():
                    copy.start()

            @pl.when(z + s < n)
            def _(k=k):
                copy = gu_copy(z + s, k, 1)
                copy.wait_recv()

                @pl.when(has_below)
                def _():
                    copy.start()

        if kinds[-1] == 0:
            return

        @pl.when((s == z) & has_above)
        def _():
            start_own_dn(0)

        @pl.when((s == n - 1 - z) & has_below)
        def _():
            start_own_dn(1)

    total_rows = groups * rows
    tall = 512 if total_rows % 512 == 0 else own_rows

    def term(slot, opening, kinds=(0, 1)):
        some = pl.ds(pl.multiple_of(slot * depth, depth), depth)

        def step(t, carry):
            where = pl.ds(pl.multiple_of(t * tall, tall), tall)
            for k in kinds:
                value = jnp.dot(normed[where, some], gbuf[k, some, :], preferred_element_type=jnp.float32)
                if opening:
                    acc[k, where, :] = value
                else:
                    acc[k, where, :] += value
            return carry

        lax.fori_loop(0, total_rows // tall, step, 0)

    def terms(s, kinds=(0, 1)):
        @pl.when(z >= s)
        def _():
            term(z - s, False, kinds)

        @pl.when(z + s < n)
        def _():
            term(z + s, False, kinds)

    gather(1)
    for i in range(1, groups):
        tok_copy(i).wait_recv()
        relay_copy(i).start()
    for i in range(1, groups):
        relay_copy(i).wait_recv()
        normalize(i, wrapped(y + groups - i, groups) * rows)
    term(z, True)
    if n > 2:
        gather(2)
    terms(1)
    if n > 2:
        terms(2)

    def later(s, carry):
        for k in range(2):
            gather(s, (k,))
            terms(s, (k,))
        return carry

    lax.fori_loop(3, n, later, 0)

    def activate(t, carry):
        where = pl.ds(pl.multiple_of(t * tile, tile), tile)
        gate_acts = acc[0, where, :]
        hidden[where, :] = (gate_acts / (1.0 + jnp.exp(-gate_acts)) * acc[1, where, :]).astype(
            jnp.bfloat16
        )
        return carry

    lax.fori_loop(0, total_rows // tile, activate, 0)

    def pair_copy(slot):
        return pltpu.make_async_remote_copy(
            src_ref=psend.at[slot],
            dst_ref=precv.at[slot],
            send_sem=pair_sent.at[slot],
            recv_sem=pair_came.at[slot],
            device_id={"tp": partner},
            device_id_type=MESH,
        )

    def mix_copy(slot, r):
        g, xx = peer(*peers[r])
        return pltpu.make_async_remote_copy(
            src_ref=asend.at[slot, g * chips + xx],
            dst_ref=arecv.at[slot, r],
            send_sem=mix_sent.at[slot * len(peers) + r],
            recv_sem=mix_came.at[slot * len(peers) + r],
            device_id={"grp": g, "tp": CORES * xx + core},
            device_id_type=MESH,
        )

    def product(slot, j, which):
        first = (CORES * j + which) * own_rows
        block = hidden[pl.ds(pl.multiple_of(first, own_rows), own_rows), :]
        return jnp.dot(block, dbuf[slot], preferred_element_type=jnp.float32)

    def block_of(slot):
        def give(j, carry):
            psend[slot, j] = product(slot, j, 1 - core).astype(jnp.bfloat16)
            return carry

        lax.fori_loop(0, groups * chips, give, 0)
        pair_copy(slot).start()

        def hold(j, carry):
            keep[j] = product(slot, j, core)
            return carry

        lax.fori_loop(0, groups * chips, hold, 0)
        pair_copy(slot).wait_recv()

        def add(j, carry):
            asend[slot, j] = (keep[j] + precv[slot, j].astype(jnp.float32)).astype(jnp.bfloat16)
            return carry

        lax.fori_loop(0, groups * chips, add, 0)
        for r in range(len(peers)):
            mix_copy(slot, r).start()

    def project(s, carry):
        @pl.when(z >= s)
        def _():
            for h in range(parts):
                copy = dn_copy(z - s, h, 0)
                copy.wait_recv()

                @pl.when(has_above)
                def _():
                    copy.start()

                block_of((z - s) * parts + h)

        @pl.when(z + s < n)
        def _():
            for h in range(parts):
                copy = dn_copy(z + s, h, 1)
                copy.wait_recv()

                @pl.when(has_below)
                def _():
                    copy.start()

                block_of((z + s) * parts + h)

        return carry

    for h in range(parts):
        block_of(z * parts + h)
    lax.fori_loop(1, n, project, 0)

    def finish(slot):
        for r in range(len(peers)):
            mix_copy(slot, r).wait_recv()
        total = asend[slot, y * chips + x].astype(jnp.float32)
        for r in range(len(peers)):
            total = total + arecv[slot, r].astype(jnp.float32)
        out[:, pl.ds(pl.multiple_of(slot * columns, columns), columns)] = total.astype(jnp.bfloat16)

    def finish_step(s, carry):
        @pl.when(z >= s)
        def _():
            for h in range(parts):
                finish((z - s) * parts + h)

        @pl.when(z + s < n)
        def _():
            for h in range(parts):
                finish((z + s) * parts + h)

        return carry

    for h in range(parts):
        finish(z * parts + h)
    lax.fori_loop(1, n, finish_step, 0)

    def left(slot, carry):
        @pl.when((slot <= z) & has_above)
        def _():
            for k in range(2):
                gu_copy(slot, k, 0).wait_send()
            for h in range(parts):
                dn_copy(slot, h, 0).wait_send()

        @pl.when((slot >= z) & has_below)
        def _():
            for k in range(2):
                gu_copy(slot, k, 1).wait_send()
            for h in range(parts):
                dn_copy(slot, h, 1).wait_send()

        for h in range(parts):
            pair_copy(slot * parts + h).wait_send()
            for r in range(len(peers)):
                mix_copy(slot * parts + h, r).wait_send()
        return carry

    lax.fori_loop(0, n, left, 0)
    for i in range(1, groups):
        tok_copy(i).wait_send()
        relay_copy(i).wait_send()


def on_device(groups, n, devices, tokens, norm_gain, gate_weight, up_weight, down_weight):
    chips = devices // CORES
    rows, width = tokens.shape
    depth, columns = gate_weight.shape[0], down_weight.shape[1]
    parts = 4 if columns % 512 == 0 else 1
    columns //= parts
    share = gate_weight.shape[1] // groups
    units = -(-share // 128) * 128
    sliced = units > share
    if sliced:
        first = lax.axis_index("grp") * share

        def mine(weight, dim):
            part = lax.dynamic_slice_in_dim(weight, first, share, dim)
            return jnp.pad(part, [(0, units - share) if d == dim else (0, 0) for d in range(2)])

        gate_weight, up_weight = mine(gate_weight, 1), mine(up_weight, 1)
        down_weight = mine(down_weight, 0)
    own_rows = rows // devices
    places, peers, blocks = groups * chips, groups * chips - 1, n * parts
    bf16, f32, dma = jnp.bfloat16, jnp.float32, pltpu.SemaphoreType.DMA
    far, near = pl.BlockSpec(memory_space=pl.ANY), pl.BlockSpec(memory_space=pltpu.VMEM)
    return pl.pallas_call(
        functools.partial(kernel, groups, n, chips, parts, sliced),
        out_shape=jax.ShapeDtypeStruct((own_rows, width), bf16),
        in_specs=[far, near, far, far, far],
        out_specs=near,
        scratch_shapes=[
            pltpu.VMEM((2, n * depth, units), bf16),
            pltpu.VMEM((blocks, units, columns), bf16),
            pltpu.VMEM((groups, rows, width), bf16),
            pltpu.VMEM((groups * rows, width), bf16),
            pltpu.VMEM((2, groups * rows, units), f32),
            pltpu.VMEM((groups * rows, units), bf16),
            pltpu.VMEM((places, own_rows, columns), f32),
            pltpu.VMEM((blocks, places, own_rows, columns), bf16),
            pltpu.VMEM((blocks, places, own_rows, columns), bf16),
            pltpu.VMEM((blocks, places, own_rows, columns), bf16),
            pltpu.VMEM((blocks, peers, own_rows, columns), bf16),
            dma((2 * n * 2,)),
            dma((n * 2,)),
            dma((2 * blocks,)),
            dma((blocks,)),
            dma((groups - 1,)),
            dma((groups - 1,)),
            dma((groups - 1,)),
            dma((groups - 1,)),
            dma((blocks,)),
            dma((blocks,)),
            dma((blocks * peers,)),
            dma((blocks * peers,)),
            dma((3 + parts,)),
        ],
        compiler_params=pltpu.CompilerParams(
            collective_id=0, has_side_effects=True, vmem_limit_bytes=VMEM_BYTES - 2**20
        ),
    )(tokens, norm_gain.reshape(1, width), gate_weight, up_weight, down_weight)


def solution(mesh):
    sizes = mesh.shape
    return jax.shard_map(
        functools.partial(on_device, sizes["grp"], sizes["fs"], sizes["tp"]),
        mesh=mesh,
        in_specs=(P(("grp", "fs"), None), P(), P("fs", "tp"), P("fs", "tp"), P("tp", "fs")),
        out_specs=P(("grp", "fs", "tp"), None),
        check_vma=False,
    )
```
